32 devices in a mesh: grp: 2 (over y), sp: 4 (over z), tp: 4 (over x, core).
Axes of the slice: x: 2, y: 2, z: 4, core: 2. Of those that a mesh axis runs over, the one named last changes fastest.
Arguments:
- stream: bfloat16 [2048, 2048], P(('grp', 'sp'), 'tp'), parts along dimension 0, may hold values from -1.5 to 1.5
- layer_norm_gain: float32 [2, 2048], replicated, may hold values from 0.1 to 1.9
- convolution_in_weight: bfloat16 [2, 2048, 1536], P(None, 'sp', 'tp'), may hold values from -0.125 to 0.125
- gating_in_weight: bfloat16 [2, 2048, 1536], P(None, 'sp', 'tp'), may hold values from -0.125 to 0.125
- output_weight: bfloat16 [2, 1536, 2048], P(None, 'tp', 'sp'), may hold values from -0.15625 to 0.15625
- convolution_kernel_taps: float32 [2, 4, 1536], P(None, None, 'tp'), may hold values from -12 to 12
- recurrent_gate_blocks: bfloat16 [2, 2, 2, 12, 128, 128], P(None, None, None, 'tp'), may hold values from -0.5 to 0.5
- channel_decay_logit: float32 [2, 2, 1536], P(None, None, 'tp')
- position_decay_boost: float32 [2, 2, 2048], P(None, None, ('grp', 'sp')), parts along dimension 2, may hold values from -1.4 to 0, as said below
Outputs:
- new_stream: bfloat16 [2048, 2048], P(('grp', 'sp'), 'tp'), parts along dimension 0
The draws below stay inside these ranges and needn't reach their ends.
There are 2 independent parts, one for each index of `grp`. The reference program is written for one: setup_inputs(seed, part) draws one part's arguments, and reference() takes and returns one part's arrays. A program takes and returns all parts, laid end to end along the dimension named above; an argument that names none is the same for every part. Nothing has to cross between parts.
Inputs may be any that keep to these rules, and one draw needn't show every extreme that they name: `position_decay_boost`: zero at all but a few positions.
All inputs are finite; a program needn't handle non-finite values.
Results may differ from the reference program's by a relative error of at most 0.025.
Values may be sent and summed in bfloat16 or wider, within the bound.
A program may use at most 128 MiB of HBM per device.

```python
import jax
import jax.numpy as jnp
from jax import lax

D = 2048
LRU = 1536
BW = 128
LAYERS = 2
TOKENS = 1024
N_TP = 4


def draw_channel_decay_logit(key, part):
    key_pick, key_slow, key_fast = jax.random.split(jax.random.fold_in(key, 11), 3)
    shape = (LAYERS, 2, LRU)
    share = 0.5
    slow = jax.random.uniform(key_pick, shape, jnp.float32) < share
    slow_rate = jax.random.uniform(key_slow, shape, jnp.float32, 0.03, 0.1) / TOKENS
    fast_rate = jnp.exp(jax.random.uniform(key_fast, shape, jnp.float32, jnp.log(0.004), jnp.log(0.0125)))
    return -jnp.log(jnp.where(slow, slow_rate, fast_rate))


def draw_position_decay_boost(key, part):
    key_spot, key_loss = jax.random.split(jax.random.fold_in(key, 23), 2)
    spots = jax.random.randint(key_spot, (LAYERS, 2, 2), 0, TOKENS)
    losses = jnp.log(jax.random.uniform(key_loss, (LAYERS, 2, 2), jnp.float32, 0.5, 0.8))
    positions = jnp.arange(TOKENS)
    return jnp.sum(jnp.where(positions[None, None, None, :] == spots[..., None], losses[..., None], 0.0), axis=2)


def draw_convolution_kernel_taps(key, part):
    noise = jax.random.normal(jax.random.fold_in(key, 37), (LAYERS, 4, LRU), jnp.float32)
    spread = jnp.array([3.0, 1.0, 1.0, 1.0], jnp.float32)
    return jnp.clip(noise * spread[None, :, None], -12.0, 12.0)


def block_levels(stream_key, extent, pieces, low, top_value):
    def one(position, blocks):
        steps = jax.random.uniform(jax.random.fold_in(jax.random.fold_in(stream_key, 6), position), (blocks,), jnp.float32, low / len(pieces), top_value / len(pieces))
        return jnp.repeat(jnp.exp(steps), extent[position] // blocks).reshape((-1,) + (1,) * (len(extent) - position - 1))

    loudness = one(*pieces[0])
    for cut in pieces[1:]:
        loudness = loudness * one(*cut)
    return loudness


def centred(own_key, extent, deviation, reach, shards=(), kind=jnp.bfloat16):
    result = deviation * jax.random.normal(own_key, extent, jnp.float32)
    if shards:
        result = result * block_levels(own_key, extent, shards, -0.22, 0.18)
    return jnp.clip(result, -reach, reach).astype(kind)


def setup_inputs(seed: int = 0, part: int = 0) -> dict:
    key_of = jax.random.split(jax.random.key(seed), 10)
    own_keys = jax.random.split(jax.random.fold_in(key_of[9], part), 10)
    stream = centred(own_keys[0], (TOKENS, D), 0.25, 1.5, ((0, 4), (1, 4)))
    layer_norm_gain = jnp.clip(1.0 + 0.18 * jax.random.normal(key_of[1], (LAYERS, D), jnp.float32), 0.1, 1.9)
    convolution_in_weight = centred(key_of[2], (LAYERS, D, LRU), D ** -0.5, 0.125, ((1, 4), (2, 4)))
    gating_in_weight = centred(key_of[3], (LAYERS, D, LRU), D ** -0.5, 0.125, ((1, 4), (2, 4)))
    output_weight = centred(key_of[4], (LAYERS, LRU, D), LRU ** -0.5, 0.15625, ((1, 4), (2, 4)))
    convolution_kernel_taps = draw_convolution_kernel_taps(jax.random.fold_in(key_of[9], 71), part)
    recurrent_gate_blocks = centred(key_of[6], (LAYERS, 2, 2, LRU // BW, BW, BW), BW ** -0.5, 0.5, ((3, 4),))
    channel_decay_logit = draw_channel_decay_logit(jax.random.fold_in(key_of[9], 71), part)
    position_decay_boost = draw_position_decay_boost(jax.random.fold_in(jax.random.fold_in(key_of[9], part), 71), part)
    return {"stream": stream, "layer_norm_gain": layer_norm_gain, "convolution_in_weight": convolution_in_weight, "gating_in_weight": gating_in_weight, "output_weight": output_weight, "convolution_kernel_taps": convolution_kernel_taps, "recurrent_gate_blocks": recurrent_gate_blocks, "channel_decay_logit": channel_decay_logit, "position_decay_boost": position_decay_boost}


EPS = 1e-06
RECURRENT_WIDTH = 8.0

def rms_norm(values, gain_row):
    floats = values.astype(jnp.float32)
    inverse = lax.rsqrt(lax.optimization_barrier(jnp.mean(floats * floats, axis=-1, keepdims=True)) + EPS)
    return (floats * inverse * gain_row.astype(jnp.float32)).astype(jnp.bfloat16)

def combine_pairs(earlier, latter):
    return (earlier[0] * latter[0], latter[0] * earlier[1] + latter[1])

def linear_recurrence(convolution_output, gate_matrix_pair, decay_logit_row, boost_row):
    seq_len = convolution_output.shape[0]
    block_width = gate_matrix_pair.shape[-1]
    conv_float = convolution_output.astype(jnp.float32)
    grouped = conv_float.reshape(seq_len, -1, block_width)
    recurrent_branch = jax.nn.sigmoid(jnp.einsum('tnc,ncd->tnd', grouped, gate_matrix_pair[0].astype(jnp.float32)).reshape(seq_len, -1))
    input_gate = jax.nn.sigmoid(jnp.einsum('tnc,ncd->tnd', grouped, gate_matrix_pair[1].astype(jnp.float32)).reshape(seq_len, -1))
    decay_logarithm = -RECURRENT_WIDTH * jax.nn.softplus(-decay_logit_row) * recurrent_branch + boost_row[:, None]
    is_start = (jnp.arange(seq_len) == 0)[:, None]
    multiplier = jnp.where(is_start, 1.0, jnp.sqrt(-jnp.expm1(2.0 * decay_logarithm)))
    driven = multiplier * input_gate * conv_float
    _, states = lax.associative_scan(combine_pairs, (jnp.exp(decay_logarithm), driven), axis=0)
    return states

def reference(stream, layer_norm_gain, convolution_in_weight, gating_in_weight, output_weight, convolution_kernel_taps, recurrent_gate_blocks, channel_decay_logit, position_decay_boost):
    seq_len = stream.shape[0]
    group_width = convolution_in_weight.shape[2] // N_TP
    for layer_index in range(LAYERS):
        normed = rms_norm(stream, layer_norm_gain[layer_index])
        proj_x = jnp.dot(normed, convolution_in_weight[layer_index], preferred_element_type=jnp.float32).astype(jnp.bfloat16)
        proj_y = jnp.dot(normed, gating_in_weight[layer_index], preferred_element_type=jnp.float32).astype(jnp.bfloat16)
        padded = jnp.pad(proj_x.astype(jnp.float32), ((1, 2), (0, 0)))
        taps_now = convolution_kernel_taps[layer_index]
        conv_mixed = taps_now[0] * padded[0:seq_len] + taps_now[1] * padded[1:seq_len + 1] + taps_now[2] * padded[2:seq_len + 2] + taps_now[3] * padded[3:seq_len + 3]
        convolution_output = conv_mixed.astype(jnp.bfloat16)
        forward_pass = linear_recurrence(convolution_output, recurrent_gate_blocks[layer_index, 0], channel_decay_logit[layer_index, 0], position_decay_boost[layer_index, 0])
        reverse_pass = jnp.flip(linear_recurrence(jnp.flip(convolution_output, 0), recurrent_gate_blocks[layer_index, 1], channel_decay_logit[layer_index, 1], jnp.flip(position_decay_boost[layer_index, 1], 0)), 0)
        gated = ((forward_pass + reverse_pass) * jax.nn.gelu(proj_y.astype(jnp.float32))).astype(jnp.bfloat16)
        branch = jnp.zeros((seq_len, stream.shape[1]), jnp.float32)
        for group in range(N_TP):
            lower = group * group_width
            partial_out = jnp.dot(gated[:, lower:lower + group_width], output_weight[layer_index, lower:lower + group_width, :], preferred_element_type=jnp.float32).astype(jnp.bfloat16)
            branch = branch + partial_out.astype(jnp.float32)
        stream = (stream.astype(jnp.float32) + branch).astype(jnp.bfloat16)
    return stream
```

```python
import jax
import jax.numpy as jnp
from jax import lax
from jax.sharding import PartitionSpec as P

EPS = 1e-06
RECURRENT_WIDTH = 8.0


def extended(cells, sides, width):
    for axis, dim in sides:
        count = lax.axis_size(axis)
        ends = count - 1
        head = lax.slice_in_dim(cells, 0, width, axis=dim)
        tail = lax.slice_in_dim(cells, cells.shape[dim] - width, cells.shape[dim], axis=dim)
        cells = jnp.concatenate(
            [
                lax.ppermute(tail, axis, [(i, (i + 1) % count) for i in range(ends)]),
                cells,
                lax.ppermute(head, axis, [((i + 1) % count, i) for i in range(ends)]),
            ],
            axis=dim,
        )
    return cells


def entering(ends, place, count):
    forward = jnp.zeros_like(ends[0, :1])
    backward = forward
    for step in range(count - 1):
        forward = jnp.where(step < place, ends[step, 0:1] * forward + ends[step, 1:2], forward)
        source = count - 1 - step
        backward = jnp.where(
            source > place, ends[source, 2:3] * backward + ends[source, 3:4], backward
        )
    return forward, backward


def rms_norm(values, gain_row):
    floats = values.astype(jnp.float32)
    inverse = lax.rsqrt(jnp.mean(floats * floats, axis=-1, keepdims=True) + EPS)
    return (floats * inverse * gain_row).astype(jnp.bfloat16)


def combine_pairs(earlier, latter):
    return (earlier[0] * latter[0], latter[0] * earlier[1] + latter[1])


def local(
    stream,
    layer_norm_gain,
    convolution_in_weight,
    gating_in_weight,
    output_weight,
    convolution_kernel_taps,
    recurrent_gate_blocks,
    channel_decay_logit,
    position_decay_boost,
):
    tok_rows = stream.shape[0]
    channels = convolution_in_weight.shape[2]
    gate_count = recurrent_gate_blocks.shape[3]
    block_width = recurrent_gate_blocks.shape[4]
    seq_devices = lax.axis_size("sp")
    my_index = lax.axis_index("sp")
    seq_length = tok_rows * seq_devices
    positions = my_index * tok_rows + lax.iota(jnp.int32, tok_rows)
    at_first = (positions == 0)[:, None]
    at_last = (positions == seq_length - 1)[:, None]
    for layer_index in range(convolution_in_weight.shape[0]):
        features = lax.all_gather(stream, "tp", axis=1, tiled=True)
        normed = rms_norm(features, layer_norm_gain[layer_index])
        acc_x = jnp.dot(
            normed,
            lax.all_gather(convolution_in_weight[layer_index], "sp", axis=0, tiled=True),
            preferred_element_type=jnp.float32,
        )
        acc_y = jnp.dot(
            normed,
            lax.all_gather(gating_in_weight[layer_index], "sp", axis=0, tiled=True),
            preferred_element_type=jnp.float32,
        )
        proj_x = acc_x.astype(jnp.bfloat16)
        proj_y = acc_y.astype(jnp.bfloat16)
        padded = extended(proj_x, (("sp", 0),), 2).astype(jnp.float32)
        taps_now = convolution_kernel_taps[layer_index]
        conv_mixed = (
            taps_now[0] * padded[1 : tok_rows + 1]
            + taps_now[1] * padded[2 : tok_rows + 2]
            + taps_now[2] * padded[3 : tok_rows + 3]
            + taps_now[3] * padded[4 : tok_rows + 4]
        )
        convolution_output = conv_mixed.astype(jnp.bfloat16)
        conv_float = convolution_output.astype(jnp.float32)
        grouped = convolution_output.reshape(tok_rows, gate_count, block_width)
        results = []
        for scan_direction in range(2):
            gate_matrix_pair = recurrent_gate_blocks[layer_index, scan_direction]
            recurrent_branch = jax.nn.sigmoid(
                jnp.einsum(
                    "tnc,ncd->tnd", grouped, gate_matrix_pair[0], preferred_element_type=jnp.float32
                ).reshape(tok_rows, channels)
            )
            input_gate = jax.nn.sigmoid(
                jnp.einsum(
                    "tnc,ncd->tnd", grouped, gate_matrix_pair[1], preferred_element_type=jnp.float32
                ).reshape(tok_rows, channels)
            )
            decay_logarithm = (
                -RECURRENT_WIDTH
                * jax.nn.softplus(-channel_decay_logit[layer_index, scan_direction])
                * recurrent_branch
                + position_decay_boost[layer_index, scan_direction][:, None]
            )
            is_start = at_first if scan_direction == 0 else at_last
            multiplier = jnp.where(is_start, 1.0, jnp.sqrt(-jnp.expm1(2.0 * decay_logarithm)))
            driven = multiplier * input_gate * conv_float
            results.append(
                lax.associative_scan(
                    combine_pairs,
                    (jnp.exp(decay_logarithm), driven),
                    reverse=scan_direction == 1,
                    axis=0,
                )
            )
        cum_fwd, local_fwd = results[0]
        cum_bwd, local_bwd = results[1]
        ends = jnp.concatenate([cum_fwd[-1:], local_fwd[-1:], cum_bwd[:1], local_bwd[:1]], axis=0)
        enter_fwd, enter_bwd = entering(lax.all_gather(ends, "sp"), my_index, seq_devices)
        state_sum = local_fwd + cum_fwd * enter_fwd + local_bwd + cum_bwd * enter_bwd
        gated = (state_sum * jax.nn.gelu(proj_y.astype(jnp.float32))).astype(jnp.bfloat16)
        partials = jnp.dot(
            gated,
            lax.all_gather(output_weight[layer_index], "sp", axis=1, tiled=True),
            preferred_element_type=jnp.float32,
        ).astype(jnp.bfloat16)
        branch_sum = lax.psum_scatter(
            partials.astype(jnp.float32).astype(jnp.bfloat16), "tp", scatter_dimension=1, tiled=True
        ).astype(jnp.float32)
        stream = (stream.astype(jnp.float32) + branch_sum).astype(jnp.bfloat16)
    return stream


def solution(mesh):
    return jax.shard_map(
        local,
        mesh=mesh,
        in_specs=(
            P(("grp", "sp"), "tp"),
            P(),
            P(None, "sp", "tp"),
            P(None, "sp", "tp"),
            P(None, "tp", "sp"),
            P(None, None, "tp"),
            P(None, None, None, "tp", None, None),
            P(None, None, "tp"),
            P(None, None, ("grp", "sp")),
        ),
        out_specs=P(("grp", "sp"), "tp"),
        check_vma=False,
    )
```

```python
import functools

import jax
import jax.numpy as jnp
from jax import lax
from jax.experimental import pallas as pl
from jax.experimental.pallas import tpu as pltpu
from jax.sharding import PartitionSpec as P

EPS = 1e-06
RECURRENT_WIDTH = 8.0
TILE = 16
HALO = 8
MESH = pl.DeviceIdType.MESH


def own_share(rows, n_grp):
    if n_grp != 2:
        return rows
    return min(rows, -(-rows * 3 // (5 * TILE)) * TILE)


def one_minus_square(log_decay, decay):
    y = 2.0 * log_decay
    series = y * (1 / 720) + 1 / 120
    series = series * y + 1 / 24
    series = series * y + 1 / 6
    series = series * y + 0.5
    series = series * y + 1.0
    return jnp.where(y > -0.25, -y * series, 1.0 - decay * decay)


def scanned(a, b, reverse):
    count = a.shape[0]
    row = lax.broadcasted_iota(jnp.int32, a.shape, 0)
    step = 1
    while step < count:
        inside = row < count - step if reverse else row >= step
        shift = count - step if reverse else step
        a_near = jnp.where(inside, pltpu.roll(a, shift, 0), 1.0)
        b_near = jnp.where(inside, pltpu.roll(b, shift, 0), 0.0)
        b = a * b_near + b
        a = a * a_near
        step *= 2
    return a, b


def kernel(
    n_grp, n_sp, n_tp,
    stream, gain, conv_w, gate_w, out_w, taps, blocks, rate, boost,
    out,
    full, normed, g_in, g_out, xpad, y_act, cum, loc, ends, gated, parts, sums,
    z_send, z_recv, y_send, y_recv, f_send, f_recv, r_send, r_recv,
    h_send, h_recv, e_send, e_recv,
):
    g, s, t = lax.axis_index("grp"), lax.axis_index("sp"), lax.axis_index("tp")
    layers = conv_w.shape[0]
    rows, ds = stream.shape
    cs, channels = conv_w.shape[1], conv_w.shape[2]
    width = blocks.shape[-1]
    weights = 3 * layers

    def remote(src, dst, send, recv, axis, place):
        return pltpu.make_async_remote_copy(
            src_ref=src, dst_ref=dst, send_sem=send, recv_sem=recv,
            device_id={axis: place}, device_id_type=MESH,
        )

    barrier = pltpu.get_barrier_semaphore()
    total = 0
    for axis, me, count in (("sp", s, n_sp), ("tp", t, n_tp), ("grp", g, n_grp)):
        for d in range(1, count):
            pl.semaphore_signal(
                barrier, inc=1, device_id={axis: lax.rem(me + d, count)}, device_id_type=MESH
            )
            total += 1
    pl.semaphore_wait(barrier, total)

    def mine(w):
        return (conv_w, gate_w, out_w)[w % 3].at[w // 3]

    def hold(w, c):
        return g_out.at[w // 3, c] if w % 3 == 2 else g_in.at[w // 3 * 2 + w % 3, c]

    def depth(w):
        return channels if w % 3 == 2 else cs

    def z_rows(w):
        share = own_share(depth(w), n_grp)
        if share == depth(w):
            return pl.ds(0, share)
        return pl.ds(pl.multiple_of(g * (depth(w) - share), TILE), share)

    def y_rows(w, place):
        share = own_share(depth(w), n_grp)
        return pl.ds(pl.multiple_of(place * share, TILE), depth(w) - share)

    def z_copy(w, c, src, to, slot):
        return remote(
            src.at[z_rows(w)], hold(w, c).at[z_rows(w)],
            z_send.at[w, slot], z_recv.at[w, c], "sp", to,
        )

    shared = n_grp == 2

    def y_copy(w, c, place):
        return remote(
            hold(w, c).at[y_rows(w, place)], hold(w, c).at[y_rows(w, place)],
            y_send.at[w, c], y_recv.at[w, c], "grp", 1 - g,
        )

    def has_y(w):
        return shared and own_share(depth(w), n_grp) < depth(w)

    def start_own(w):
        @pl.when(s < n_sp - 1)
        def _():
            z_copy(w, s, mine(w), s + 1, s).start()

        @pl.when(s > 0)
        def _():
            z_copy(w, s, mine(w), s - 1, n_sp).start()

    def pass_on(w, c, onward, to, back):
        z_copy(w, c, hold(w, c), back, c).wait_recv()

        @pl.when(onward)
        def _():
            z_copy(w, c, hold(w, c), to, c).start()

        if has_y(w):
            y_copy(w, c, g).start()

    def event(w, k):
        @pl.when(s - 1 - k >= 0)
        def _():
            pass_on(w, s - 1 - k, s < n_sp - 1, s + 1, s - 1)

        @pl.when(s + 1 + k <= n_sp - 1)
        def _():
            pass_on(w, s + 1 + k, s > 0, s - 1, s + 1)

        if k == 0 and w + 2 < weights:
            start_own(w + 2)

    queue = [(w, k) for w in range(weights) for k in range(n_sp - 1)]

    def serve(count):
        for _ in range(min(count, len(queue))):
            event(*queue.pop(0))

    def serve_until(w):
        while queue and queue[0][0] <= w:
            event(*queue.pop(0))

    def landed(w):
        if has_y(w):
            for c in range(n_sp):
                @pl.when(c != s)
                def _():
                    y_copy(w, c, 1 - g).wait_recv()

    def f_copy(layer, src, source, d, to):
        return remote(
            src, full.at[layer, source], f_send.at[layer, d], f_recv.at[layer, source], "tp", to
        )

    tp_order = [d for d in range(1, n_tp)]

    def send_features(layer, src):
        for d in tp_order:
            f_copy(layer, src, t, d, lax.rem(t + d, n_tp)).start()

    send_features(0, stream)
    for w in range(min(2, weights)):
        start_own(w)
    full[0, t] = stream[...]
    for w in range(weights):
        if w % 3 == 2:
            g_out[w // 3, s] = out_w[w // 3]
        else:
            g_in[w // 3 * 2 + w % 3, s] = (conv_w, gate_w)[w % 3][w // 3]

    row = lax.broadcasted_iota(jnp.int32, (rows, 1), 0)

    for layer in range(layers):
        if layer == 0:
            serve(1)
        for d in tp_order:
            source = lax.rem(t + d, n_tp)
            f_copy(layer, full.at[layer, source], source, d, source).wait_recv()
        square = jnp.zeros((rows, 1), jnp.float32)
        for j in range(n_tp):
            x = full[layer, j].astype(jnp.float32)
            square += jnp.sum(x * x, axis=-1, keepdims=True)
        inverse = lax.rsqrt(square / (n_tp * ds) + EPS)
        piece = min(cs, ds)
        for p in range(n_tp * ds // piece):
            at = p * piece
            x = full[layer, at // ds, :, at % ds : at % ds + piece].astype(jnp.float32)
            x = x * inverse * gain[layer : layer + 1, at : at + piece]
            normed[at // cs, :, at % cs : at % cs + piece] = x.astype(jnp.bfloat16)

        def project(w):
            acc = None
            for c in range(n_sp):
                term = jnp.dot(
                    normed[c], g_in[w // 3 * 2 + w % 3, c], preferred_element_type=jnp.float32
                )
                acc = term if acc is None else acc + term
            return acc.astype(jnp.bfloat16).astype(jnp.float32)

        wx, wy, wo = 3 * layer, 3 * layer + 1, 3 * layer + 2
        serve_until(wx)
        if layer == 0:
            serve(1)
        landed(wx)
        xpad[layer, HALO : HALO + rows] = project(wx)

        def halo_right():
            return remote(
                xpad.at[layer, pl.ds(rows, HALO)], xpad.at[layer, pl.ds(0, HALO)],
                h_send.at[layer, 0], h_recv.at[layer, 0], "sp", lax.rem(s + 1, n_sp),
            )

        def halo_left():
            return remote(
                xpad.at[layer, pl.ds(HALO, HALO)], xpad.at[layer, pl.ds(HALO + rows, HALO)],
                h_send.at[layer, 1], h_recv.at[layer, 1], "sp", lax.rem(s + n_sp - 1, n_sp),
            )

        @pl.when(s < n_sp - 1)
        def _():
            halo_right().start()

        @pl.when(s > 0)
        def _():
            halo_left().start()

        serve_until(wy)
        landed(wy)
        y_act[...] = jax.nn.gelu(project(wy))

        @pl.when(s > 0)
        def _():
            halo_right().wait_recv()

        @pl.when(s == 0)
        def _():
            xpad[layer, 0:HALO] = jnp.zeros((HALO, channels), jnp.float32)

        @pl.when(s < n_sp - 1)
        def _():
            halo_left().wait_recv()

        @pl.when(s == n_sp - 1)
        def _():
            xpad[layer, HALO + rows : 2 * HALO + rows] = jnp.zeros((HALO, channels), jnp.float32)

        for n in range(channels // width):
            lanes = slice(n * width, (n + 1) * width)
            conv = None
            for k in range(taps.shape[1]):
                term = taps[layer, k : k + 1, lanes] * xpad[
                    layer, HALO - 1 + k : HALO - 1 + k + rows, lanes
                ]
                conv = term if conv is None else conv + term
            conv_half = conv.astype(jnp.bfloat16)
            conv = conv_half.astype(jnp.float32)
            for d in range(2):
                recur = jax.nn.sigmoid(
                    jnp.dot(conv_half, blocks[layer, d, 0, n], preferred_element_type=jnp.float32)
                )
                inject = jax.nn.sigmoid(
                    jnp.dot(conv_half, blocks[layer, d, 1, n], preferred_element_type=jnp.float32)
                )
                at = 2 * layer + d
                log_decay = rate[at : at + 1, lanes] * recur + boost[:, at : at + 1]
                decay = jnp.exp(log_decay)
                first = (row == 0) & (s == 0) if d == 0 else (row == rows - 1) & (s == n_sp - 1)
                m = jnp.where(first, 1.0, jnp.sqrt(one_minus_square(log_decay, decay)))
                a, b = scanned(decay, m * inject * conv, d == 1)
                cum[d, :, lanes] = a
                loc[d, :, lanes] = b
                edge = rows - 1 if d == 0 else 0
                ends[layer, s, 2 * d : 2 * d + 1, lanes] = a[edge : edge + 1]
                ends[layer, s, 2 * d + 1 : 2 * d + 2, lanes] = b[edge : edge + 1]
            serve(1)

        def e_copy(source, d, to):
            return remote(
                ends.at[layer, source], ends.at[layer, source],
                e_send.at[layer, d], e_recv.at[layer, source], "sp", to,
            )

        for d in range(1, n_sp):
            e_copy(s, d, lax.rem(s + d, n_sp)).start()
        serve_until(wo)
        for d in range(1, n_sp):
            source = lax.rem(s + d, n_sp)
            e_copy(source, d, source).wait_recv()
        forward = jnp.zeros((1, channels), jnp.float32)
        backward = forward
        for step in range(n_sp - 1):
            forward = jnp.where(
                step < s, ends[layer, step, 0:1] * forward + ends[layer, step, 1:2], forward
            )
            back = n_sp - 1 - step
            backward = jnp.where(
                back > s, ends[layer, back, 2:3] * backward + ends[layer, back, 3:4], backward
            )
        state = loc[0] + cum[0] * forward + loc[1] + cum[1] * backward
        gated[...] = (state * y_act[...]).astype(jnp.bfloat16)

        def r_copy(source, slot, to):
            return remote(
                parts.at[layer, to], sums.at[layer, source],
                r_send.at[layer, slot], r_recv.at[layer, source], "tp", to,
            )

        landed(wo)
        for c in range(n_sp):
            partial = jnp.dot(gated[...], g_out[layer, c], preferred_element_type=jnp.float32)
            partial = partial.astype(jnp.bfloat16)
            for q in range(cs // piece):
                at = c * cs + q * piece
                j = at // ds
                parts[layer, j, :, at % ds : at % ds + piece] = partial[
                    :, q * piece : (q + 1) * piece
                ]
                if (at + piece) % ds == 0:
                    @pl.when(j != t)
                    def _():
                        r_copy(t, j, j).start()

        if layer == 0:
            serve(n_sp - 1)
        new = full[layer, t].astype(jnp.float32) + parts[layer, t].astype(jnp.float32)
        for d in tp_order:
            source = lax.rem(t + d, n_tp)
            r_copy(source, source, source).wait_recv()
            new = new + sums[layer, source].astype(jnp.float32)
        new = new.astype(jnp.bfloat16)
        if layer + 1 < layers:
            full[layer + 1, t] = new
            send_features(layer + 1, full.at[layer + 1, t])
        else:
            out[...] = new

    for w in range(weights):
        @pl.when(s < n_sp - 1)
        def _():
            z_copy(w, s, mine(w), s + 1, s).wait_send()

        @pl.when(s > 0)
        def _():
            z_copy(w, s, mine(w), s - 1, n_sp).wait_send()

        for c in range(n_sp):
            @pl.when(((c < s) & (s < n_sp - 1)) | ((c > s) & (s > 0)))
            def _():
                z_copy(w, c, hold(w, c), lax.rem(s + 1, n_sp), c).wait_send()

            if has_y(w):
                @pl.when(c != s)
                def _():
                    y_copy(w, c, g).wait_send()

    for layer in range(layers):
        for d in tp_order:
            f_copy(layer, full.at[layer, t], t, d, lax.rem(t + d, n_tp)).wait_send()
        for j in range(n_tp):
            @pl.when(j != t)
            def _():
                remote(
                    parts.at[layer, j], sums.at[layer, t],
                    r_send.at[layer, j], r_recv.at[layer, t], "tp", j,
                ).wait_send()

        for d in range(1, n_sp):
            remote(
                ends.at[layer, s], ends.at[layer, s],
                e_send.at[layer, d], e_recv.at[layer, s], "sp", lax.rem(s + d, n_sp),
            ).wait_send()

        @pl.when(s < n_sp - 1)
        def _():
            remote(
                xpad.at[layer, pl.ds(rows, HALO)], xpad.at[layer, pl.ds(0, HALO)],
                h_send.at[layer, 0], h_recv.at[layer, 0], "sp", lax.rem(s + 1, n_sp),
            ).wait_send()

        @pl.when(s > 0)
        def _():
            remote(
                xpad.at[layer, pl.ds(HALO, HALO)], xpad.at[layer, pl.ds(HALO + rows, HALO)],
                h_send.at[layer, 1], h_recv.at[layer, 1], "sp", lax.rem(s + n_sp - 1, n_sp),
            ).wait_send()


def solution(mesh):
    n_grp, n_sp, n_tp = mesh.shape["grp"], mesh.shape["sp"], mesh.shape["tp"]

    def local(stream, gain, conv_w, gate_w, out_w, taps, blocks, logit, boost):
        layers, cs, channels = conv_w.shape
        rows, ds = stream.shape
        rate = (-RECURRENT_WIDTH * jax.nn.softplus(-logit)).reshape(-1, channels)
        boost = boost.reshape(-1, rows).T
        bf, f32, dma = jnp.bfloat16, jnp.float32, pltpu.SemaphoreType.DMA
        vmem = pltpu.VMEM
        return pl.pallas_call(
            functools.partial(kernel, n_grp, n_sp, n_tp),
            out_shape=jax.ShapeDtypeStruct((rows, ds), bf),
            in_specs=[pl.BlockSpec(memory_space=vmem)] * 9,
            out_specs=pl.BlockSpec(memory_space=vmem),
            scratch_shapes=[
                vmem((layers, n_tp, rows, ds), bf),
                vmem((n_sp, rows, cs), bf),
                vmem((2 * layers, n_sp, cs, channels), bf),
                vmem((layers, n_sp, channels, cs), bf),
                vmem((layers, rows + 2 * HALO, channels), f32),
                vmem((rows, channels), f32),
                vmem((2, rows, channels), f32),
                vmem((2, rows, channels), f32),
                vmem((layers, n_sp, 8, channels), f32),
                vmem((rows, channels), bf),
                vmem((layers, n_tp, rows, ds), bf),
                vmem((layers, n_tp, rows, ds), bf),
                dma((3 * layers, n_sp + 1)),
                dma((3 * layers, n_sp)),
                dma((3 * layers, n_sp)),
                dma((3 * layers, n_sp)),
                dma((layers, n_tp)),
                dma((layers, n_tp)),
                dma((layers, n_tp)),
                dma((layers, n_tp)),
                dma((layers, 2)),
                dma((layers, 2)),
                dma((layers, n_sp)),
                dma((layers, n_sp)),
            ],
            compiler_params=pltpu.CompilerParams(
                collective_id=0, has_side_effects=True, vmem_limit_bytes=60 * 1024 * 1024
            ),
        )(stream, gain, conv_w, gate_w, out_w, taps, blocks, rate, boost)

    return jax.shard_map(
        local,
        mesh=mesh,
        in_specs=(
            P(("grp", "sp"), "tp"),
            P(),
            P(None, "sp", "tp"),
            P(None, "sp", "tp"),
            P(None, "tp", "sp"),
            P(None, None, "tp"),
            P(None, None, None, "tp", None, None),
            P(None, None, "tp"),
            P(None, None, ("grp", "sp")),
        ),
        out_specs=P(("grp", "sp"), "tp"),
        check_vma=False,
    )
```

```python
import functools

import jax
import jax.numpy as jnp
from jax import lax
from jax.experimental import pallas as pl
from jax.experimental.pallas import tpu as pltpu
from jax.sharding import PartitionSpec as P

EPS = 1e-06
RECURRENT_WIDTH = 8.0
TILE = 16
HALO = 8
MESH = pl.DeviceIdType.MESH


def own_share(rows, n_grp):
    if n_grp != 2:
        return rows
    return min(rows, -(-rows * 11 // (20 * TILE)) * TILE)


def one_minus_square(log_decay, decay):
    y = 2.0 * log_decay
    series = y * (1 / 720) + 1 / 120
    series = series * y + 1 / 24
    series = series * y + 1 / 6
    series = series * y + 0.5
    series = series * y + 1.0
    return jnp.where(y > -0.25, -y * series, 1.0 - decay * decay)


def scanned(a, b, reverse):
    count = a.shape[0]
    row = lax.broadcasted_iota(jnp.int32, a.shape, 0)
    step = 1
    while step < count:
        inside = row < count - step if reverse else row >= step
        shift = count - step if reverse else step
        a_near = jnp.where(inside, pltpu.roll(a, shift, 0), 1.0)
        b_near = jnp.where(inside, pltpu.roll(b, shift, 0), 0.0)
        b = a * b_near + b
        a = a * a_near
        step *= 2
    return a, b


def kernel(
    n_grp, n_sp, n_tp,
    stream, gain, conv_w, gate_w, out_w, taps, blocks, rate, boost,
    out,
    full, normed, g_in, g_out, xpad, y_act, cum, loc, ends, gated, parts, sums,
    z_send, z_recv, y_send, y_recv, f_send, f_recv, r_send, r_recv,
    h_send, h_recv, e_send, e_recv,
):
    g, s, t = lax.axis_index("grp"), lax.axis_index("sp"), lax.axis_index("tp")
    layers = conv_w.shape[0]
    rows, ds = stream.shape
    cs, channels = conv_w.shape[1], conv_w.shape[2]
    width = blocks.shape[-1]
    weights = 3 * layers

    def remote(src, dst, send, recv, axis, place):
        return pltpu.make_async_remote_copy(
            src_ref=src, dst_ref=dst, send_sem=send, recv_sem=recv,
            device_id={axis: place}, device_id_type=MESH,
        )

    barrier = pltpu.get_barrier_semaphore()
    total = 0
    for axis, me, count in (("sp", s, n_sp), ("tp", t, n_tp), ("grp", g, n_grp)):
        for d in range(1, count):
            pl.semaphore_signal(
                barrier, inc=1, device_id={axis: lax.rem(me + d, count)}, device_id_type=MESH
            )
            total += 1
    pl.semaphore_wait(barrier, total)

    def mine(w):
        return (conv_w, gate_w, out_w)[w % 3].at[w // 3]

    def hold(w, c):
        return g_out.at[w // 3, c] if w % 3 == 2 else g_in.at[w // 3 * 2 + w % 3, c]

    def depth(w):
        return channels if w % 3 == 2 else cs

    def z_rows(w):
        share = own_share(depth(w), n_grp)
        if share == depth(w):
            return pl.ds(0, share)
        return pl.ds(pl.multiple_of(g * (depth(w) - share), TILE), share)

    def y_rows(w, place):
        share = own_share(depth(w), n_grp)
        return pl.ds(pl.multiple_of(place * share, TILE), depth(w) - share)

    def z_copy(w, c, src, to, slot):
        return remote(
            src.at[z_rows(w)], hold(w, c).at[z_rows(w)],
            z_send.at[w, slot], z_recv.at[w, c], "sp", to,
        )

    shared = n_grp == 2

    def y_copy(w, c, place):
        return remote(
            hold(w, c).at[y_rows(w, place)], hold(w, c).at[y_rows(w, place)],
            y_send.at[w, c], y_recv.at[w, c], "grp", 1 - g,
        )

    def has_y(w):
        return shared and own_share(depth(w), n_grp) < depth(w)

    def start_own(w):
        @pl.when(s < n_sp - 1)
        def _():
            z_copy(w, s, mine(w), s + 1, s).start()

        @pl.when(s > 0)
        def _():
            z_copy(w, s, mine(w), s - 1, n_sp).start()

    def pass_on(w, c, onward, to, back):
        z_copy(w, c, hold(w, c), back, c).wait_recv()

        @pl.when(onward)
        def _():
            z_copy(w, c, hold(w, c), to, c).start()

        if has_y(w):
            y_copy(w, c, g).start()

    def event(w, k):
        @pl.when(s - 1 - k >= 0)
        def _():
            pass_on(w, s - 1 - k, s < n_sp - 1, s + 1, s - 1)

        @pl.when(s + 1 + k <= n_sp - 1)
        def _():
            pass_on(w, s + 1 + k, s > 0, s - 1, s + 1)

        if k == 0 and w + 2 < weights:
            start_own(w + 2)

    queue = [(w, k) for w in range(weights) for k in range(n_sp - 1)]

    def serve(count):
        for _ in range(min(count, len(queue))):
            event(*queue.pop(0))

    def serve_until(w):
        while queue and queue[0][0] <= w:
            event(*queue.pop(0))

    def landed(w):
        if has_y(w):
            for c in range(n_sp):
                @pl.when(c != s)
                def _():
                    y_copy(w, c, 1 - g).wait_recv()

    def f_copy(layer, src, source, d, to):
        return remote(
            src, full.at[layer, source], f_send.at[layer, d], f_recv.at[layer, source], "tp", to
        )

    tp_order = [d for d in range(1, n_tp)]

    def send_features(layer, src):
        for d in tp_order:
            f_copy(layer, src, t, d, lax.rem(t + d, n_tp)).start()

    send_features(0, stream)
    for w in range(min(2, weights)):
        start_own(w)
    full[0, t] = stream[...]
    for w in range(weights):
        if w % 3 == 2:
            g_out[w // 3, s] = out_w[w // 3]
        else:
            g_in[w // 3 * 2 + w % 3, s] = (conv_w, gate_w)[w % 3][w // 3]

    row = lax.broadcasted_iota(jnp.int32, (rows, 1), 0)

    for layer in range(layers):
        if layer == 0:
            serve(1)
        for d in tp_order:
            source = lax.rem(t + d, n_tp)
            f_copy(layer, full.at[layer, source], source, d, source).wait_recv()
        square = jnp.zeros((rows, 1), jnp.float32)
        for j in range(n_tp):
            x = full[layer, j].astype(jnp.float32)
            square += jnp.sum(x * x, axis=-1, keepdims=True)
        inverse = lax.rsqrt(square / (n_tp * ds) + EPS)
        piece = min(cs, ds)
        for p in range(n_tp * ds // piece):
            at = p * piece
            x = full[layer, at // ds, :, at % ds : at % ds + piece].astype(jnp.float32)
            x = x * inverse * gain[layer : layer + 1, at : at + piece]
            normed[at // cs, :, at % cs : at % cs + piece] = x.astype(jnp.bfloat16)

        def project(w):
            acc = None
            for c in range(n_sp):
                term = jnp.dot(
                    normed[c], g_in[w // 3 * 2 + w % 3, c], preferred_element_type=jnp.float32
                )
                acc = term if acc is None else acc + term
            return acc.astype(jnp.bfloat16).astype(jnp.float32)

        wx, wy, wo = 3 * layer, 3 * layer + 1, 3 * layer + 2
        serve_until(wx)
        if layer == 0:
            serve(1)
        landed(wx)
        xpad[layer, HALO : HALO + rows] = project(wx)

        def halo_right():
            return remote(
                xpad.at[layer, pl.ds(rows, HALO)], xpad.at[layer, pl.ds(0, HALO)],
                h_send.at[layer, 0], h_recv.at[layer, 0], "sp", lax.rem(s + 1, n_sp),
            )

        def halo_left():
            return remote(
                xpad.at[layer, pl.ds(HALO, HALO)], xpad.at[layer, pl.ds(HALO + rows, HALO)],
                h_send.at[layer, 1], h_recv.at[layer, 1], "sp", lax.rem(s + n_sp - 1, n_sp),
            )

        @pl.when(s < n_sp - 1)
        def _():
            halo_right().start()

        @pl.when(s > 0)
        def _():
            halo_left().start()

        serve_until(wy)
        landed(wy)
        y_act[...] = jax.nn.gelu(project(wy))

        @pl.when(s > 0)
        def _():
            halo_right().wait_recv()

        @pl.when(s == 0)
        def _():
            xpad[layer, 0:HALO] = jnp.zeros((HALO, channels), jnp.float32)

        @pl.when(s < n_sp - 1)
        def _():
            halo_left().wait_recv()

        @pl.when(s == n_sp - 1)
        def _():
            xpad[layer, HALO + rows : 2 * HALO + rows] = jnp.zeros((HALO, channels), jnp.float32)

        for n in range(channels // width):
            lanes = slice(n * width, (n + 1) * width)
            conv = None
            for k in range(taps.shape[1]):
                term = taps[layer, k : k + 1, lanes] * xpad[
                    layer, HALO - 1 + k : HALO - 1 + k + rows, lanes
                ]
                conv = term if conv is None else conv + term
            conv_half = conv.astype(jnp.bfloat16)
            conv = conv_half.astype(jnp.float32)
            for d in range(2):
                recur = jax.nn.sigmoid(
                    jnp.dot(conv_half, blocks[layer, d, 0, n], preferred_element_type=jnp.float32)
                )
                inject = jax.nn.sigmoid(
                    jnp.dot(conv_half, blocks[layer, d, 1, n], preferred_element_type=jnp.float32)
                )
                at = 2 * layer + d
                log_decay = rate[at : at + 1, lanes] * recur + boost[:, at : at + 1]
                decay = jnp.exp(log_decay)
                first = (row == 0) & (s == 0) if d == 0 else (row == rows - 1) & (s == n_sp - 1)
                m = jnp.where(first, 1.0, jnp.sqrt(one_minus_square(log_decay, decay)))
                a, b = scanned(decay, m * inject * conv, d == 1)
                cum[d, :, lanes] = a
                loc[d, :, lanes] = b
                edge = rows - 1 if d == 0 else 0
                ends[layer, s, 2 * d : 2 * d + 1, lanes] = a[edge : edge + 1]
                ends[layer, s, 2 * d + 1 : 2 * d + 2, lanes] = b[edge : edge + 1]
            serve(1)

        def e_copy(source, d, to):
            return remote(
                ends.at[layer, source], ends.at[layer, source],
                e_send.at[layer, d], e_recv.at[layer, source], "sp", to,
            )

        for d in range(1, n_sp):
            e_copy(s, d, lax.rem(s + d, n_sp)).start()
        serve_until(wo)
        for d in range(1, n_sp):
            source = lax.rem(s + d, n_sp)
            e_copy(source, d, source).wait_recv()
        forward = jnp.zeros((1, channels), jnp.float32)
        backward = forward
        for step in range(n_sp - 1):
            forward = jnp.where(
                step < s, ends[layer, step, 0:1] * forward + ends[layer, step, 1:2], forward
            )
            back = n_sp - 1 - step
            backward = jnp.where(
                back > s, ends[layer, back, 2:3] * backward + ends[layer, back, 3:4], backward
            )
        state = loc[0] + cum[0] * forward + loc[1] + cum[1] * backward
        gated[...] = (state * y_act[...]).astype(jnp.bfloat16)

        def r_copy(source, slot, to):
            return remote(
                parts.at[layer, to], sums.at[layer, source],
                r_send.at[layer, slot], r_recv.at[layer, source], "tp", to,
            )

        landed(wo)
        for c in range(n_sp):
            partial = jnp.dot(gated[...], g_out[layer, c], preferred_element_type=jnp.float32)
            partial = partial.astype(jnp.bfloat16)
            for q in range(cs // piece):
                at = c * cs + q * piece
                j = at // ds
                parts[layer, j, :, at % ds : at % ds + piece] = partial[
                    :, q * piece : (q + 1) * piece
                ]
                if (at + piece) % ds == 0:
                    @pl.when(j != t)
                    def _():
                        r_copy(t, j, j).start()

        if layer == 0:
            serve(n_sp - 1)
        new = full[layer, t].astype(jnp.float32) + parts[layer, t].astype(jnp.float32)
        for d in tp_order:
            source = lax.rem(t + d, n_tp)
            r_copy(source, source, source).wait_recv()
            new = new + sums[layer, source].astype(jnp.float32)
        new = new.astype(jnp.bfloat16)
        if layer + 1 < layers:
            full[layer + 1, t] = new
            send_features(layer + 1, full.at[layer + 1, t])
        else:
            out[...] = new

    for w in range(weights):
        @pl.when(s < n_sp - 1)
        def _():
            z_copy(w, s, mine(w), s + 1, s).wait_send()

        @pl.when(s > 0)
        def _():
            z_copy(w, s, mine(w), s - 1, n_sp).wait_send()

        for c in range(n_sp):
            @pl.when(((c < s) & (s < n_sp - 1)) | ((c > s) & (s > 0)))
            def _():
                z_copy(w, c, hold(w, c), lax.rem(s + 1, n_sp), c).wait_send()

            if has_y(w):
                @pl.when(c != s)
                def _():
                    y_copy(w, c, g).wait_send()

    for layer in range(layers):
        for d in tp_order:
            f_copy(layer, full.at[layer, t], t, d, lax.rem(t + d, n_tp)).wait_send()
        for j in range(n_tp):
            @pl.when(j != t)
            def _():
                remote(
                    parts.at[layer, j], sums.at[layer, t],
                    r_send.at[layer, j], r_recv.at[layer, t], "tp", j,
                ).wait_send()

        for d in range(1, n_sp):
            remote(
                ends.at[layer, s], ends.at[layer, s],
                e_send.at[layer, d], e_recv.at[layer, s], "sp", lax.rem(s + d, n_sp),
            ).wait_send()

        @pl.when(s < n_sp - 1)
        def _():
            remote(
                xpad.at[layer, pl.ds(rows, HALO)], xpad.at[layer, pl.ds(0, HALO)],
                h_send.at[layer, 0], h_recv.at[layer, 0], "sp", lax.rem(s + 1, n_sp),
            ).wait_send()

        @pl.when(s > 0)
        def _():
            remote(
                xpad.at[layer, pl.ds(HALO, HALO)], xpad.at[layer, pl.ds(HALO + rows, HALO)],
                h_send.at[layer, 1], h_recv.at[layer, 1], "sp", lax.rem(s + n_sp - 1, n_sp),
            ).wait_send()


def solution(mesh):
    n_grp, n_sp, n_tp = mesh.shape["grp"], mesh.shape["sp"], mesh.shape["tp"]

    def local(stream, gain, conv_w, gate_w, out_w, taps, blocks, logit, boost):
        layers, cs, channels = conv_w.shape
        rows, ds = stream.shape
        rate = (-RECURRENT_WIDTH * jax.nn.softplus(-logit)).reshape(-1, channels)
        boost = boost.reshape(-1, rows).T
        bf, f32, dma = jnp.bfloat16, jnp.float32, pltpu.SemaphoreType.DMA
        vmem = pltpu.VMEM
        return pl.pallas_call(
            functools.partial(kernel, n_grp, n_sp, n_tp),
            out_shape=jax.ShapeDtypeStruct((rows, ds), bf),
            in_specs=[pl.BlockSpec(memory_space=vmem)] * 9,
            out_specs=pl.BlockSpec(memory_space=vmem),
            scratch_shapes=[
                vmem((layers, n_tp, rows, ds), bf),
                vmem((n_sp, rows, cs), bf),
                vmem((2 * layers, n_sp, cs, channels), bf),
                vmem((layers, n_sp, channels, cs), bf),
                vmem((layers, rows + 2 * HALO, channels), f32),
                vmem((rows, channels), f32),
                vmem((2, rows, channels), f32),
                vmem((2, rows, channels), f32),
                vmem((layers, n_sp, 8, channels), f32),
                vmem((rows, channels), bf),
                vmem((layers, n_tp, rows, ds), bf),
                vmem((layers, n_tp, rows, ds), bf),
                dma((3 * layers, n_sp + 1)),
                dma((3 * layers, n_sp)),
                dma((3 * layers, n_sp)),
                dma((3 * layers, n_sp)),
                dma((layers, n_tp)),
                dma((layers, n_tp)),
                dma((layers, n_tp)),
                dma((layers, n_tp)),
                dma((layers, 2)),
                dma((layers, 2)),
                dma((layers, n_sp)),
                dma((layers, n_sp)),
            ],
            compiler_params=pltpu.CompilerParams(
                collective_id=0, has_side_effects=True, vmem_limit_bytes=60 * 1024 * 1024
            ),
        )(stream, gain, conv_w, gate_w, out_w, taps, blocks, rate, boost)

    return jax.shard_map(
        local,
        mesh=mesh,
        in_specs=(
            P(("grp", "sp"), "tp"),
            P(),
            P(None, "sp", "tp"),
            P(None, "sp", "tp"),
            P(None, "tp", "sp"),
            P(None, None, "tp"),
            P(None, None, None, "tp", None, None),
            P(None, None, "tp"),
            P(None, None, ("grp", "sp")),
        ),
        out_specs=P(("grp", "sp"), "tp"),
        check_vma=False,
    )
```
